32 devices in a mesh: grp: 2 (over y), sp: 4 (over z), tp: 4 (over x, core).
Axes of the slice: x: 2, y: 2, z: 4, core: 2. Of those that a mesh axis runs over, the one named last changes fastest.
Arguments:
- conv_input: bfloat16 [4096, 1024], P(('grp', 'sp'), 'tp'), parts along dimension 0, may hold values from -6 to 6
- pre_gate: bfloat16 [4096, 1024], P(('grp', 'sp'), 'tp'), parts along dimension 0, may hold values from -6 to 6
- post_gate: bfloat16 [4096, 1024], P(('grp', 'sp'), 'tp'), parts along dimension 0, may hold values from -6 to 6
- conv_taps: float32 [3, 1024], replicated, may hold values from -3.5 to 3.5
- out_proj: bfloat16 [1024, 2048], replicated, may hold values from -0.1875 to 0.1875
- residual_in: bfloat16 [4096, 2048], P(('grp', 'sp', 'tp')), parts along dimension 0, may hold values from -6 to 6
- norm_gain: float32 [2048], replicated, may hold values from 0.1 to 1.9
- routes: int32 [4096, 2], P(('grp', 'sp', 'tp')), parts along dimension 0, may hold values from 0 to 7, as said below
- route_weight: float32 [4096, 2], P(('grp', 'sp', 'tp')), parts along dimension 0, may hold values from 0.1 to 1
- w_gate: bfloat16 [8, 2048, 1024], P('sp', None, 'tp'), may hold values from -0.125 to 0.125
- w_up: bfloat16 [8, 2048, 1024], P('sp', None, 'tp'), may hold values from -0.125 to 0.125
- w_down: bfloat16 [8, 1024, 2048], P('sp', 'tp'), may hold values from -0.1875 to 0.1875
Outputs:
- layer_out: bfloat16 [4096, 2048], P(('grp', 'sp', 'tp')), parts along dimension 0
The draws below stay inside these ranges and needn't reach their ends.
There are 2 independent parts, one for each index of `grp`. The reference program is written for one: setup_inputs(seed, part) draws one part's arguments, and reference() takes and returns one part's arrays. A program takes and returns all parts, laid end to end along the dimension named above; an argument that names none is the same for every part. Nothing has to cross between parts.
Inputs may be any that keep to these rules, and one draw needn't show every extreme that they name: `routes`: the two numbers of a row differ and lie in the same group of 2 consecutive experts. In each aligned block of 128 rows every expert is named exactly 32 times.
All inputs are finite; a program needn't handle non-finite values.
Results may differ from the reference program's by a relative error of at most 0.0085.
Values may be sent and summed in bfloat16 or wider, within the bound.
A program may use at most 64 MiB of HBM per device.

```python
import jax
import jax.numpy as jnp
from jax import lax

D = 2048
CH = 1024
HID = 1024
CONV = 3
GROUPS = 4
TOKENS = 2048
EXPERTS = 8
EPG = 2
ROW_BLOCK = 128
BLOCKS = 16
N_TP = 4


def draw_routes(key, part):
    base = jax.random.fold_in(key, 7)
    perm_key, shift_key = jax.random.split(base)
    block_keys = jax.random.split(perm_key, BLOCKS)
    ranks = jax.vmap(lambda k: jax.random.permutation(k, ROW_BLOCK))(block_keys).astype(jnp.int32)
    offsets = jax.random.randint(shift_key, (BLOCKS, 1), 0, EPG // 2).astype(jnp.int32)
    group = ranks % GROUPS
    within = ranks // GROUPS
    first = 2 * within % EPG
    second = (2 * within + 1 + 2 * offsets) % EPG
    chosen = jnp.stack([group * EPG + first, group * EPG + second], axis=-1)
    return chosen.reshape(TOKENS, 2).astype(jnp.int32)


def block_scale(own_key, shape, cuts, least, high):
    level = 1.0
    for position, shards_of in cuts:
        steps = jax.random.uniform(jax.random.fold_in(jax.random.fold_in(own_key, 6), position), (shards_of,), jnp.float32, least / len(cuts), high / len(cuts))
        level = level * jnp.repeat(jnp.exp(steps), shape[position] // shards_of).reshape((-1,) + (1,) * (len(shape) - 1 - position))
    return level


def gaussian(rng, dims, spread, most, pieces=(), held_as=jnp.bfloat16):
    entries = spread * jax.random.normal(rng, dims, jnp.float32)
    if pieces:
        entries = entries * block_scale(rng, dims, pieces, -0.22, 0.18)
    return jnp.clip(entries, -most, most).astype(held_as)


def setup_inputs(seed: int = 0, part: int = 0) -> dict:
    key_of = jax.random.split(jax.random.key(seed), 13)
    part_splits = jax.random.split(jax.random.fold_in(key_of[12], part), 13)
    conv_input = gaussian(part_splits[0], (TOKENS, CH), 1.0, 6.0, ((0, 4), (1, 4)))
    pre_gate = gaussian(part_splits[1], (TOKENS, CH), 1.0, 6.0, ((0, 4), (1, 4)))
    post_gate = gaussian(part_splits[2], (TOKENS, CH), 1.0, 6.0, ((0, 4), (1, 4)))
    conv_taps = gaussian(key_of[3], (CONV, CH), CONV ** -0.5, 3.5, (), jnp.float32)
    out_proj = gaussian(key_of[4], (CH, D), CH ** -0.5, 0.1875)
    residual_in = gaussian(part_splits[5], (TOKENS, D), 1.0, 6.0, ((0, 16),))
    norm_gain = jnp.clip(1.0 + 0.18 * jax.random.normal(key_of[6], (D,), jnp.float32), 0.1, 1.9)
    routes = draw_routes(jax.random.fold_in(jax.random.fold_in(key_of[12], part), 71), part)
    route_weight = jnp.clip(0.1 + 0.9 * jax.random.uniform(part_splits[8], (TOKENS, 2), jnp.float32) ** block_scale(part_splits[8], (TOKENS, 2), ((0, 16),), -0.2, 0.2), 0.1, 1.0)
    w_gate = gaussian(key_of[9], (EXPERTS, D, HID), D ** -0.5, 0.125, ((0, 4), (2, 4)))
    w_up = gaussian(key_of[10], (EXPERTS, D, HID), D ** -0.5, 0.125, ((0, 4), (2, 4)))
    w_down = gaussian(key_of[11], (EXPERTS, HID, D), HID ** -0.5, 0.1875, ((0, 4), (1, 4)))
    return dict(conv_input=conv_input, pre_gate=pre_gate, post_gate=post_gate, conv_taps=conv_taps, out_proj=out_proj, residual_in=residual_in, norm_gain=norm_gain, routes=routes, route_weight=route_weight, w_gate=w_gate, w_up=w_up, w_down=w_down)


def reference(conv_input, pre_gate, post_gate, conv_taps, out_proj, residual_in, norm_gain, routes, route_weight, w_gate, w_up, w_down):
    gated = pre_gate.astype(jnp.float32) * conv_input.astype(jnp.float32)
    padded = jnp.pad(gated, ((2, 0), (0, 0)))
    conv = padded[2:] * conv_taps[2] + padded[1:-1] * conv_taps[1] + padded[:-2] * conv_taps[0]
    mixed = (post_gate.astype(jnp.float32) * conv).astype(jnp.bfloat16)
    projected = jnp.dot(mixed, out_proj, preferred_element_type=jnp.float32)
    stream = residual_in.astype(jnp.float32) + projected
    scale = lax.rsqrt(lax.optimization_barrier(jnp.mean(stream * stream, axis=-1, keepdims=True)) + 1e-06)
    normed = (stream * scale * norm_gain).astype(jnp.bfloat16)
    flat_routes = routes.reshape(-1)
    per_expert = TOKENS * 2 // EXPERTS
    hid_shard = HID // N_TP

    def one_expert(carry, expert):
        picked = jnp.nonzero(flat_routes == expert, size=per_expert)[0].astype(jnp.int32)
        rows = normed[picked // 2]
        gate_all = w_gate[expert]
        up_all = w_up[expert]
        down_all = w_down[expert]
        total = jnp.zeros((per_expert, D), jnp.float32)
        for shard in range(N_TP):
            low = shard * hid_shard
            gate = jnp.dot(rows, gate_all[:, low:low + hid_shard], preferred_element_type=jnp.float32)
            upper = jnp.dot(rows, up_all[:, low:low + hid_shard], preferred_element_type=jnp.float32)
            hidden = (jax.nn.silu(gate) * upper).astype(jnp.bfloat16)
            part = jnp.dot(hidden, down_all[low:low + hid_shard], preferred_element_type=jnp.float32).astype(jnp.bfloat16)
            part = lax.optimization_barrier(part)
            total = total + part.astype(jnp.float32)
        carry = carry.at[picked].set(total.astype(jnp.bfloat16))
        return (carry, None)
    start = jnp.zeros((TOKENS * 2, D), jnp.bfloat16)
    outputs, _ = lax.scan(one_expert, start, jnp.arange(EXPERTS, dtype=jnp.int32))
    expert_out = outputs.reshape(TOKENS, 2, D).astype(jnp.float32)
    weighted = lax.optimization_barrier(jnp.sum(route_weight[:, :, None] * expert_out, axis=1))
    return (stream + weighted).astype(jnp.bfloat16)
```

```python
import functools

import jax
import jax.numpy as jnp
from jax import lax
from jax.experimental import pallas as pl
from jax.experimental.pallas import tpu as pltpu
from jax.sharding import PartitionSpec as P

GROUPS = 4
LANES = 128
F32, BF16 = jnp.float32, jnp.bfloat16


def shifted(block, axis, distance):
    devices = range(lax.axis_size(axis))
    route = [(i - distance, i) for i in devices if i - distance in devices]
    return lax.ppermute(block, axis, route)


def generic(
    conv_input,
    pre_gate,
    post_gate,
    conv_taps,
    out_proj,
    residual_in,
    norm_gain,
    routes,
    route_weight,
    w_gate,
    w_up,
    w_down,
):
    shards = lax.axis_size("tp")
    place = lax.axis_index("tp")
    seq_ranks = lax.axis_size("sp")
    channels = conv_input.shape[1]
    width = residual_in.shape[1]
    taps = lax.dynamic_slice_in_dim(conv_taps, place * channels, channels, 1)
    prior_input, prior_gate = shifted((conv_input[-2:], pre_gate[-2:]), "sp", 1)
    gated = jnp.concatenate(
        [
            prior_gate.astype(jnp.float32) * prior_input.astype(jnp.float32),
            pre_gate.astype(jnp.float32) * conv_input.astype(jnp.float32),
        ],
        axis=0,
    )
    conv = gated[2:] * taps[2] + gated[1:-1] * taps[1] + gated[:-2] * taps[0]
    mixed = (post_gate.astype(jnp.float32) * conv).astype(jnp.bfloat16)
    token_rows = lax.all_to_all(mixed, "tp", split_axis=0, concat_axis=1, tiled=True)
    projected = jnp.dot(token_rows, out_proj, preferred_element_type=jnp.float32)
    stream = residual_in.astype(jnp.float32) + projected
    scale = lax.rsqrt(jnp.mean(stream * stream, axis=-1, keepdims=True) + 1e-06)
    normed = (stream * scale * norm_gain).astype(jnp.bfloat16)
    block_rows = routes.shape[0]
    local_experts = w_gate.shape[0]
    experts = local_experts * seq_ranks
    capacity = 2 * block_rows // experts
    flat_routes = routes.reshape(-1)
    position = jnp.arange(flat_routes.shape[0], dtype=jnp.int32)
    earlier = (flat_routes[:, None] == flat_routes[None, :]) & (
        position[None, :] < position[:, None]
    )
    rank = jnp.sum(earlier.astype(jnp.int32), axis=1)
    slot = flat_routes * capacity + rank
    outgoing = (
        jnp.zeros((experts * capacity, width), jnp.bfloat16).at[slot].set(normed[position // 2])
    )
    outgoing = outgoing.reshape(seq_ranks, local_experts, capacity, width)
    spread = lax.all_gather(
        lax.all_to_all(outgoing, "sp", split_axis=0, concat_axis=0, tiled=True)[:, None],
        "tp",
        axis=1,
        tiled=True,
    )
    count = spread.shape[3]
    partials = []
    for expert in range(local_experts):
        rows = spread[:, :, expert].reshape(seq_ranks * shards * count, width)
        gate = jnp.dot(rows, w_gate[expert], preferred_element_type=jnp.float32)
        upper = jnp.dot(rows, w_up[expert], preferred_element_type=jnp.float32)
        hidden = (jax.nn.silu(gate) * upper).astype(jnp.bfloat16)
        part = jnp.dot(hidden, w_down[expert], preferred_element_type=jnp.float32).astype(
            jnp.bfloat16
        )
        partials.append(part.reshape(seq_ranks, shards, count, width))
    stacked = jnp.stack(partials, axis=2)
    summed = lax.psum_scatter(stacked, "tp", scatter_dimension=1, tiled=True).astype(jnp.float32)
    returned = lax.all_to_all(
        summed[:, 0].astype(jnp.bfloat16), "sp", split_axis=0, concat_axis=0, tiled=True
    )
    results = returned.reshape(experts * capacity, width)[slot]
    results = results.reshape(block_rows, 2, width).astype(jnp.float32)
    weighted = jnp.sum(route_weight[:, :, None] * results, axis=1)
    return (stream + weighted).astype(jnp.bfloat16)


def dot(a, b):
    return jnp.dot(a, b, preferred_element_type=F32)


def fused_kernel(
    conv_input,
    pre_gate,
    post_gate,
    conv_taps,
    proj_hbm,
    residual,
    gain,
    routes,
    route_weight,
    gate_hbm,
    up_hbm,
    down_hbm,
    out,
    proj,
    w_gate,
    w_up,
    w_down,
    halo,
    gated,
    mix_out,
    mix_in,
    stream,
    leaving,
    tok,
    hidden,
    part,
    from_core,
    kept,
    to_chip,
    from_chip,
    to_home,
    home,
    load_sem,
    halo_send,
    halo_recv,
    mix_send,
    mix_recv,
    z_send,
    z_recv,
    x_send,
    x_recv,
    c_send,
    c_recv,
    d_send,
    d_recv,
    one_send,
    one_recv,
    two_send,
    two_recv,
    home_send,
    home_recv,
):
    s, t = lax.axis_index("sp"), lax.axis_index("tp")
    rows, width = residual.shape
    channels = conv_input.shape[1]
    cap = rows // GROUPS
    units = w_gate.shape[2]
    core, chip, far = t + 1 - 2 * (t % 2), (t + 2) % 4, 3 - t
    sp_of = [s, s + 1 - 2 * (s % 2), (s + 2) % 4, 3 - s]
    pos = lambda place: (place % 2) * 2 + place // 2
    block = lambda place: pl.ds(pl.multiple_of(pos(place) * cap, cap), cap)
    pending = []

    def send(src, dst, send_sem, recv_sem, **where):
        copy = pltpu.make_async_remote_copy(
            src_ref=src,
            dst_ref=dst,
            send_sem=send_sem,
            recv_sem=recv_sem,
            device_id=where,
            device_id_type=pl.DeviceIdType.MESH,
        )
        copy.start()
        pending.append(copy)
        return copy

    loads = []
    for i, (a, b) in enumerate(
        ((proj_hbm, proj), (gate_hbm, w_gate), (up_hbm, w_up), (down_hbm, w_down))
    ):
        loads.append(pltpu.make_async_copy(a, b, load_sem.at[i]))
        loads[-1].start()

    barrier = pltpu.get_barrier_semaphore()
    for other in (core, chip, far):
        pl.semaphore_signal(
            barrier, inc=1, device_id={"tp": other}, device_id_type=pl.DeviceIdType.MESH
        )
    for other in sp_of[1:]:
        pl.semaphore_signal(
            barrier, inc=1, device_id={"sp": other}, device_id_type=pl.DeviceIdType.MESH
        )
    pl.semaphore_wait(barrier, 6)

    count = conv_input.shape[0]
    halo_copies = [
        send(
            ref.at[pl.ds(count - 16, 16), :],
            halo.at[i],
            halo_send.at[i],
            halo_recv.at[i],
            sp=(s + 1) % 4,
        )
        for i, ref in enumerate((conv_input, pre_gate))
    ]
    gated[pl.ds(8, count), :] = pre_gate[...].astype(F32) * conv_input[...].astype(F32)
    taps = conv_taps[:, pl.ds(pl.multiple_of(t * channels, channels), channels)]
    for copy in halo_copies:
        copy.wait_recv()
    before = halo[0, 8:16, :].astype(F32) * halo[1, 8:16, :].astype(F32)
    gated[0:8, :] = jnp.where(s > 0, before, 0.0)

    def mix(place):
        start = pl.multiple_of(place * rows, rows)
        g = gated[pl.ds(start, rows + 8), :]
        conv = g[8:] * taps[2:3] + g[7:-1] * taps[1:2] + g[6:-2] * taps[0:1]
        return (post_gate[pl.ds(start, rows), :].astype(F32) * conv).astype(BF16)

    mix_copies = []
    for i, place in enumerate((chip, far, core)):
        mix_out[i] = mix(place)
        mix_copies.append(
            send(mix_out.at[i], mix_in.at[t], mix_send.at[i], mix_recv.at[i], tp=place)
        )
    mix_in[t] = mix(t)

    first, second = routes[:, 0:1], routes[:, 1:2]
    lane = lax.broadcasted_iota(jnp.int32, (rows, LANES), 1)
    epg = w_gate.shape[0]
    member = (first >= lane * epg) & (first < lane * epg + epg) & (lane < GROUPS)
    down = lax.broadcasted_iota(jnp.int32, (rows, rows), 0)
    across = lax.broadcasted_iota(jnp.int32, (rows, rows), 1)
    earlier = jnp.where(across < down, 1.0, 0.0).astype(BF16)
    member = jnp.where(member, 1.0, 0.0)
    rank = dot(earlier, member.astype(BF16))
    slot = jnp.sum(member * (rank + (lane * cap).astype(F32)), axis=1, keepdims=True)
    back = jnp.where(slot == across.astype(F32), 1.0, 0.0)
    pick = back.T.astype(BF16)
    back = back.astype(BF16)
    low = jnp.where(first < second, route_weight[:, 0:1], route_weight[:, 1:2])
    high = jnp.where(first < second, route_weight[:, 1:2], route_weight[:, 0:1])
    low_top, high_top = low.astype(BF16).astype(F32), high.astype(BF16).astype(F32)
    scales = jnp.where(
        lane == 0,
        low_top,
        jnp.where(
            lane == 1,
            low - low_top,
            jnp.where(lane == 2, high_top, jnp.where(lane == 3, high - high_top, 0.0)),
        ),
    ).astype(BF16)
    leaving[:, pl.ds(width, LANES)] = dot(pick, scales).astype(BF16)

    loads[0].wait()
    for copy in mix_copies:
        copy.wait_recv()
    tile = 512

    def project(n, squares):
        cols = pl.ds(pl.multiple_of(n * tile, tile), tile)
        total = residual[:, cols].astype(F32)
        for j in range(4):
            total += dot(mix_in[j], proj[pl.ds(j * channels, channels), cols])
        stream[:, cols] = total
        return squares + jnp.sum(total * total, axis=1, keepdims=True)

    squares = lax.fori_loop(0, width // tile, project, jnp.zeros((rows, 1), F32))
    scale = lax.rsqrt(squares / width + 1e-06)

    def norm(n, carry):
        cols = pl.ds(pl.multiple_of(n * tile, tile), tile)
        row = (stream[:, cols] * scale * gain[:, cols]).astype(BF16)
        leaving[:, cols] = dot(pick, row).astype(BF16)
        return carry

    lax.fori_loop(0, width // tile, norm, 0)

    group_rows = lambda g: pl.ds(pl.multiple_of(g * cap, cap), cap)
    z_copies = [None]
    for k in (1, 2, 3):
        g = sp_of[k]
        z_copies.append(
            send(
                leaving.at[group_rows(g), :],
                tok.at[s, block(t), :],
                z_send.at[k],
                z_recv.at[k],
                sp=g,
            )
        )
    x_copies, c_copies, d_copies = [], [], []

    def forward(k):
        src = leaving.at[group_rows(s), :]
        if k:
            z_copies[k].wait_recv()
            src = tok.at[sp_of[k], block(t), :]
        dst = tok.at[sp_of[k], block(t), :]
        x_copies.append(send(src, dst, x_send.at[k], x_recv.at[k], tp=chip))
        c_copies.append(send(src, dst, c_send.at[k], c_recv.at[k], tp=core))

    forward(0)
    tok[s, block(t), :] = leaving[group_rows(s), :]
    for load in loads[1:]:
        load.wait()

    def compute(k):
        g = sp_of[k]
        x = tok[g, :, 0:width]
        for e in range(epg):
            w = tok[g, :, pl.ds(width, LANES)].astype(F32)
            w = w[:, 2 * e : 2 * e + 1] + w[:, 2 * e + 1 : 2 * e + 2]
            gate = dot(x, w_gate[e])
            upper = dot(x, w_up[e])
            act = gate / (1.0 + jnp.exp(-gate)) * upper * w
            hidden[:, pl.ds(e * units, units)] = act.astype(BF16)

        def lower(n, carry):
            cols = pl.ds(pl.multiple_of(n * tile, tile), tile)
            part[k, :, cols] = dot(hidden[...], w_down[:, cols]).astype(BF16)
            return carry

        lax.fori_loop(0, width // tile, lower, 0)

    half = 2 * cap
    core_rows = lambda c: pl.ds(pl.multiple_of(c * half, half), half)
    one_copies, two_copies, home_copies = [], [], []

    def stage_one(k):
        one_copies.append(
            send(
                part.at[k, core_rows(1 - t % 2), :],
                from_core.at[k],
                one_send.at[k],
                one_recv.at[k],
                tp=core,
            )
        )

    def stage_two(k):
        one_copies[k].wait_recv()
        for mine in (False, True):
            x = t // 2 if mine else 1 - t // 2
            base = pl.multiple_of((t % 2) * half + x * cap, cap)
            near = pl.multiple_of(x * cap, cap)
            total = part[k, pl.ds(base, cap), :].astype(F32)
            total += from_core[k, pl.ds(near, cap), :].astype(F32)
            if mine:
                kept[k] = total
            else:
                to_chip[k] = total.astype(BF16)
                two_copies.append(
                    send(to_chip.at[k], from_chip.at[k], two_send.at[k], two_recv.at[k], tp=chip)
                )

    def stage_three(k):
        two_copies[k].wait_recv()
        total = (kept[k] + from_chip[k].astype(F32)).astype(BF16)
        if k == 0:
            home[group_rows(s), :] = total
            home_copies.append(None)
        else:
            to_home[k] = total
            home_copies.append(
                send(
                    to_home.at[k],
                    home.at[group_rows(s), :],
                    home_send.at[k],
                    home_recv.at[k],
                    sp=sp_of[k],
                )
            )

    for k in range(4):
        if k + 1 < 4:
            forward(k + 1)
        x_copies[k].wait_recv()
        arrived = tok.at[sp_of[k], block(chip), :]
        d_copies.append(send(arrived, arrived, d_send.at[k], d_recv.at[k], tp=core))
        if k >= 1:
            stage_two(k - 1)
        c_copies[k].wait_recv()
        d_copies[k].wait_recv()
        compute(k)
        stage_one(k)
        if k >= 2:
            stage_three(k - 2)
    stage_two(3)
    stage_three(2)
    stage_three(3)
    for copy in home_copies[1:]:
        copy.wait_recv()

    def finish(n, carry):
        cols = pl.ds(pl.multiple_of(n * tile, tile), tile)
        out[:, cols] = (stream[:, cols] + dot(back, home[:, cols])).astype(BF16)
        return carry

    lax.fori_loop(0, width // tile, finish, 0)
    for copy in pending:
        copy.wait_send()


def fused(*args):
    (conv_input, _, _, _, out_proj, residual, gain, _, _, w_gate, w_up, w_down) = args
    rows, width = residual.shape
    count, channels = conv_input.shape
    local, _, units = w_gate.shape
    cap = rows // GROUPS
    w_down = w_down.reshape(local * units, width)
    args = args[:6] + (gain.reshape(1, width),) + args[7:11] + (w_down,)
    vmem = pl.BlockSpec(memory_space=pltpu.VMEM)
    far = pl.BlockSpec(memory_space=pl.ANY)
    sems = pltpu.SemaphoreType.DMA
    return pl.pallas_call(
        fused_kernel,
        out_shape=jax.ShapeDtypeStruct((rows, width), BF16),
        in_specs=[vmem] * 4 + [far] + [vmem] * 4 + [far] * 3,
        out_specs=vmem,
        scratch_shapes=[
            pltpu.VMEM(out_proj.shape, BF16),
            pltpu.VMEM(w_gate.shape, BF16),
            pltpu.VMEM(w_up.shape, BF16),
            pltpu.VMEM(w_down.shape, BF16),
            pltpu.VMEM((2, 16, channels), BF16),
            pltpu.VMEM((count + 8, channels), F32),
            pltpu.VMEM((3, rows, channels), BF16),
            pltpu.VMEM((4, rows, channels), BF16),
            pltpu.VMEM((rows, width), F32),
            pltpu.VMEM((rows, width + LANES), BF16),
            pltpu.VMEM((4, 4 * cap, width + LANES), BF16),
            pltpu.VMEM((4 * cap, local * units), BF16),
            pltpu.VMEM((4, 4 * cap, width), BF16),
            pltpu.VMEM((4, 2 * cap, width), BF16),
            pltpu.VMEM((4, cap, width), F32),
            pltpu.VMEM((4, cap, width), BF16),
            pltpu.VMEM((4, cap, width), BF16),
            pltpu.VMEM((4, cap, width), BF16),
            pltpu.VMEM((rows, width), BF16),
            sems((4,)),
            sems((2,)),
            sems((2,)),
            sems((3,)),
            sems((3,)),
        ]
        + [sems((4,))] * 14,
        compiler_params=pltpu.CompilerParams(
            collective_id=0, has_side_effects=True, vmem_limit_bytes=56 << 20
        ),
    )(*args)


def on_device(*args):
    residual, routes, w_gate = args[5], args[7], args[9]
    rows, local, seq_ranks = residual.shape[0], w_gate.shape[0], lax.axis_size("sp")
    dense = local == routes.shape[1] == 2 and local * seq_ranks == local * GROUPS
    if dense and lax.axis_size("tp") == 4 and rows % LANES == 0:
        return fused(*args)
    return generic(*args)


def solution(mesh):
    return jax.shard_map(
        on_device,
        mesh=mesh,
        in_specs=(
            P(("grp", "sp"), "tp"),
            P(("grp", "sp"), "tp"),
            P(("grp", "sp"), "tp"),
            P(),
            P(),
            P(("grp", "sp", "tp"), None),
            P(),
            P(("grp", "sp", "tp"), None),
            P(("grp", "sp", "tp"), None),
            P("sp", None, "tp"),
            P("sp", None, "tp"),
            P("sp", "tp", None),
        ),
        out_specs=P(("grp", "sp", "tp"), None),
        check_vma=False,
    )
```

```python
import functools

import jax
import jax.numpy as jnp
from jax import lax
from jax.experimental import pallas as pl
from jax.experimental.pallas import tpu as pltpu
from jax.sharding import PartitionSpec as P

GROUPS = 4
LANES = 128
F32, BF16 = jnp.float32, jnp.bfloat16


def shifted(block, axis, distance):
    devices = range(lax.axis_size(axis))
    route = [(i - distance, i) for i in devices if i - distance in devices]
    return lax.ppermute(block, axis, route)


def generic(
    conv_input,
    pre_gate,
    post_gate,
    conv_taps,
    out_proj,
    residual_in,
    norm_gain,
    routes,
    route_weight,
    w_gate,
    w_up,
    w_down,
):
    shards = lax.axis_size("tp")
    place = lax.axis_index("tp")
    seq_ranks = lax.axis_size("sp")
    channels = conv_input.shape[1]
    width = residual_in.shape[1]
    taps = lax.dynamic_slice_in_dim(conv_taps, place * channels, channels, 1)
    prior_input, prior_gate = shifted((conv_input[-2:], pre_gate[-2:]), "sp", 1)
    gated = jnp.concatenate(
        [
            prior_gate.astype(jnp.float32) * prior_input.astype(jnp.float32),
            pre_gate.astype(jnp.float32) * conv_input.astype(jnp.float32),
        ],
        axis=0,
    )
    conv = gated[2:] * taps[2] + gated[1:-1] * taps[1] + gated[:-2] * taps[0]
    mixed = (post_gate.astype(jnp.float32) * conv).astype(jnp.bfloat16)
    token_rows = lax.all_to_all(mixed, "tp", split_axis=0, concat_axis=1, tiled=True)
    projected = jnp.dot(token_rows, out_proj, preferred_element_type=jnp.float32)
    stream = residual_in.astype(jnp.float32) + projected
    scale = lax.rsqrt(jnp.mean(stream * stream, axis=-1, keepdims=True) + 1e-06)
    normed = (stream * scale * norm_gain).astype(jnp.bfloat16)
    block_rows = routes.shape[0]
    local_experts = w_gate.shape[0]
    experts = local_experts * seq_ranks
    capacity = 2 * block_rows // experts
    flat_routes = routes.reshape(-1)
    position = jnp.arange(flat_routes.shape[0], dtype=jnp.int32)
    earlier = (flat_routes[:, None] == flat_routes[None, :]) & (
        position[None, :] < position[:, None]
    )
    rank = jnp.sum(earlier.astype(jnp.int32), axis=1)
    slot = flat_routes * capacity + rank
    outgoing = (
        jnp.zeros((experts * capacity, width), jnp.bfloat16).at[slot].set(normed[position // 2])
    )
    outgoing = outgoing.reshape(seq_ranks, local_experts, capacity, width)
    spread = lax.all_gather(
        lax.all_to_all(outgoing, "sp", split_axis=0, concat_axis=0, tiled=True)[:, None],
        "tp",
        axis=1,
        tiled=True,
    )
    count = spread.shape[3]
    partials = []
    for expert in range(local_experts):
        rows = spread[:, :, expert].reshape(seq_ranks * shards * count, width)
        gate = jnp.dot(rows, w_gate[expert], preferred_element_type=jnp.float32)
        upper = jnp.dot(rows, w_up[expert], preferred_element_type=jnp.float32)
        hidden = (jax.nn.silu(gate) * upper).astype(jnp.bfloat16)
        part = jnp.dot(hidden, w_down[expert], preferred_element_type=jnp.float32).astype(
            jnp.bfloat16
        )
        partials.append(part.reshape(seq_ranks, shards, count, width))
    stacked = jnp.stack(partials, axis=2)
    summed = lax.psum_scatter(stacked, "tp", scatter_dimension=1, tiled=True).astype(jnp.float32)
    returned = lax.all_to_all(
        summed[:, 0].astype(jnp.bfloat16), "sp", split_axis=0, concat_axis=0, tiled=True
    )
    results = returned.reshape(experts * capacity, width)[slot]
    results = results.reshape(block_rows, 2, width).astype(jnp.float32)
    weighted = jnp.sum(route_weight[:, :, None] * results, axis=1)
    return (stream + weighted).astype(jnp.bfloat16)


def dot(a, b):
    return jnp.dot(a, b, preferred_element_type=F32)


def fused_kernel(
    input_hbm,
    pre_hbm,
    post_hbm,
    conv_taps,
    proj_hbm,
    residual_hbm,
    gain,
    routes,
    route_weight,
    gate_hbm,
    up_hbm,
    down_hbm,
    out,
    conv_input,
    pre_gate,
    post_gate,
    residual,
    proj,
    w_gate,
    w_up,
    w_down,
    halo,
    gated,
    mix_out,
    mix_in,
    stream,
    leaving,
    tok,
    hidden,
    part,
    from_core,
    kept,
    to_chip,
    from_chip,
    to_home,
    home,
    load_sem,
    halo_send,
    halo_recv,
    mix_send,
    mix_recv,
    z_send,
    z_recv,
    x_send,
    x_recv,
    c_send,
    c_recv,
    d_send,
    d_recv,
    one_send,
    one_recv,
    two_send,
    two_recv,
    home_send,
    home_recv,
):
    s, t = lax.axis_index("sp"), lax.axis_index("tp")
    rows, width = residual.shape
    channels = conv_input.shape[1]
    cap = rows // GROUPS
    units = w_gate.shape[2]
    core, chip, far = t + 1 - 2 * (t % 2), (t + 2) % 4, 3 - t
    sp_of = [s, s + 1 - 2 * (s % 2), (s + 2) % 4, 3 - s]
    pos = lambda place: (place % 2) * 2 + place // 2
    block = lambda place: pl.ds(pl.multiple_of(pos(place) * cap, cap), cap)
    pending = []

    def send(src, dst, send_sem, recv_sem, **where):
        copy = pltpu.make_async_remote_copy(
            src_ref=src,
            dst_ref=dst,
            send_sem=send_sem,
            recv_sem=recv_sem,
            device_id=where,
            device_id_type=pl.DeviceIdType.MESH,
        )
        copy.start()
        pending.append(copy)
        return copy

    barrier = pltpu.get_barrier_semaphore()
    for other in (core, chip, far):
        pl.semaphore_signal(
            barrier, inc=1, device_id={"tp": other}, device_id_type=pl.DeviceIdType.MESH
        )
    for other in sp_of[1:]:
        pl.semaphore_signal(
            barrier, inc=1, device_id={"sp": other}, device_id_type=pl.DeviceIdType.MESH
        )
    loads = []
    for i, (a, b) in enumerate(
        (
            (input_hbm, conv_input),
            (pre_hbm, pre_gate),
            (post_hbm, post_gate),
            (residual_hbm, residual),
            (proj_hbm, proj),
            (gate_hbm, w_gate),
            (up_hbm, w_up),
            (down_hbm, w_down),
        )
    ):
        loads.append(pltpu.make_async_copy(a, b, load_sem.at[i]))
        loads[-1].start()

    first, second = routes[0:1, :], routes[1:2, :]
    epg = w_gate.shape[0]
    down = lax.broadcasted_iota(jnp.int32, (rows, rows), 0)
    across = lax.broadcasted_iota(jnp.int32, (rows, rows), 1)
    group = lax.broadcasted_iota(jnp.int32, (16, rows), 0)
    member = (first >= group * epg) & (first < group * epg + epg) & (group < GROUPS)
    member = jnp.where(member, 1.0, 0.0)
    earlier = jnp.where(down < across, 1.0, 0.0).astype(BF16)
    rank = dot(member.astype(BF16), earlier)
    slot = jnp.sum(member * (rank + (group * cap).astype(F32)), axis=0, keepdims=True)
    pick = jnp.where(slot == down.astype(F32), 1.0, 0.0)
    back = pick.T.astype(BF16)
    pick = pick.astype(BF16)
    low = jnp.where(first < second, route_weight[0:1, :], route_weight[1:2, :])
    high = jnp.where(first < second, route_weight[1:2, :], route_weight[0:1, :])
    low_top, high_top = low.astype(BF16).astype(F32), high.astype(BF16).astype(F32)
    line = lax.broadcasted_iota(jnp.int32, (LANES, rows), 0)
    scales = jnp.where(
        line == 0,
        low_top,
        jnp.where(
            line == 1,
            low - low_top,
            jnp.where(line == 2, high_top, jnp.where(line == 3, high - high_top, 0.0)),
        ),
    ).astype(BF16)
    scales = lax.dot_general(
        pick, scales, (((1,), (1,)), ((), ())), preferred_element_type=F32
    )
    leaving[:, pl.ds(width, LANES)] = scales.astype(BF16)

    loads[0].wait()
    loads[1].wait()
    pl.semaphore_wait(barrier, 6)

    count = conv_input.shape[0]
    halo_copies = [
        send(
            ref.at[pl.ds(count - 16, 16), :],
            halo.at[i],
            halo_send.at[i],
            halo_recv.at[i],
            sp=(s + 1) % 4,
        )
        for i, ref in enumerate((conv_input, pre_gate))
    ]
    gated[pl.ds(8, count), :] = pre_gate[...].astype(F32) * conv_input[...].astype(F32)
    taps = conv_taps[:, pl.ds(pl.multiple_of(t * channels, channels), channels)]
    loads[2].wait()

    def mix(place):
        start = pl.multiple_of(place * rows, rows)
        g = gated[pl.ds(start, rows + 8), :]
        conv = g[8:] * taps[2:3] + g[7:-1] * taps[1:2] + g[6:-2] * taps[0:1]
        return (post_gate[pl.ds(start, rows), :].astype(F32) * conv).astype(BF16)

    def send_mixed(i, place):
        mix_out[i] = mix(place)
        send(mix_out.at[i], mix_in.at[t], mix_send.at[i], mix_recv.at[t], tp=place)

    def wait_mixed(place):
        pltpu.make_async_remote_copy(
            src_ref=mix_in.at[place],
            dst_ref=mix_in.at[place],
            send_sem=mix_send.at[0],
            recv_sem=mix_recv.at[place],
            device_id={"tp": place},
            device_id_type=pl.DeviceIdType.MESH,
        ).wait_recv()

    across_chip = 2 * (1 - t // 2)
    send_mixed(0, across_chip + 1)
    for copy in halo_copies:
        copy.wait_recv()
    before = halo[0, 8:16, :].astype(F32) * halo[1, 8:16, :].astype(F32)
    gated[0:8, :] = jnp.where(s > 0, before, 0.0)
    send_mixed(1, across_chip)
    send_mixed(2, core)
    mix_in[t] = mix(t)

    tile = 512
    tiles = width // tile
    column = lambda n: pl.ds(pl.multiple_of(n * tile, tile), tile)
    weights_of = lambda place: pl.ds(pl.multiple_of(place * channels, channels), channels)
    loads[3].wait()
    loads[4].wait()
    wait_mixed(core)

    def project_near(n, carry):
        cols = column(n)
        total = residual[:, cols].astype(F32)
        for place in (t, core):
            total += dot(mix_in[place], proj[weights_of(place), cols])
        stream[:, cols] = total
        return carry

    lax.fori_loop(0, tiles, project_near, 0)
    wait_mixed(chip)
    wait_mixed(far)

    def project_far(n, squares):
        cols = column(n)
        total = stream[:, cols]
        for place in (chip, far):
            total += dot(mix_in[place], proj[weights_of(place), cols])
        stream[:, cols] = total
        return squares + jnp.sum(total * total, axis=1, keepdims=True)

    squares = lax.fori_loop(0, tiles, project_far, jnp.zeros((rows, 1), F32))
    scale = lax.rsqrt(squares / width + 1e-06)

    def norm(n, carry):
        cols = column(n)
        row = (stream[:, cols] * scale * gain[:, cols]).astype(BF16)
        leaving[:, cols] = dot(pick, row).astype(BF16)
        return carry

    split = width // 2
    halves = (pl.ds(0, split), pl.ds(split, split))
    sent = (pl.ds(0, split), pl.ds(split, split + LANES))
    group_rows = lambda g: pl.ds(pl.multiple_of(g * cap, cap), cap)
    z_copies, x_copies, c_copies, d_copies = {}, {}, {}, {}
    one_copies, two_copies, home_copies = {}, {}, {}

    def forward(k, h):
        src = leaving.at[group_rows(s), sent[h]]
        if k:
            z_copies[k, h].wait_recv()
            src = tok.at[sp_of[k], block(t), sent[h]]
        dst = tok.at[sp_of[k], block(t), sent[h]]
        i = 2 * k + h
        x_copies[k, h] = send(src, dst, x_send.at[i], x_recv.at[i], tp=chip)
        c_copies[k, h] = send(src, dst, c_send.at[i], c_recv.at[i], tp=core)

    def pass_on(k, h):
        x_copies[k, h].wait_recv()
        i = 2 * k + h
        arrived = tok.at[sp_of[k], block(chip), sent[h]]
        d_copies[k, h] = send(arrived, arrived, d_send.at[i], d_recv.at[i], tp=core)

    for h in (0, 1):
        lax.fori_loop(h * tiles // 2, (h + 1) * tiles // 2, norm, 0)
        for k in (1, 2, 3):
            i = 2 * k + h
            z_copies[k, h] = send(
                leaving.at[group_rows(sp_of[k]), sent[h]],
                tok.at[s, block(t), sent[h]],
                z_send.at[i],
                z_recv.at[i],
                sp=sp_of[k],
            )
        forward(0, h)
    tok[s, block(t), :] = leaving[group_rows(s), :]
    for load in loads[5:]:
        load.wait()

    def raise_units(k):
        g = sp_of[k]
        for h in (0, 1):
            c_copies[k, h].wait_recv()
            d_copies[k, h].wait_recv()
        x = tok[g, :, 0:width]
        for e in range(epg):
            w = tok[g, :, pl.ds(width, LANES)].astype(F32)
            w = w[:, 2 * e : 2 * e + 1] + w[:, 2 * e + 1 : 2 * e + 2]
            gate = dot(x, w_gate[e])
            upper = dot(x, w_up[e])
            act = gate / (1.0 + jnp.exp(-gate)) * upper * w
            hidden[:, pl.ds(e * units, units)] = act.astype(BF16)

    both = 2 * cap
    core_rows = lambda c: pl.ds(pl.multiple_of(c * both, both), both)

    def lower_units(k, h):
        def lower(n, carry):
            cols = column(n)
            part[k, :, cols] = dot(hidden[...], w_down[:, cols]).astype(BF16)
            return carry

        lax.fori_loop(h * tiles // 2, (h + 1) * tiles // 2, lower, 0)
        i = 2 * k + h
        one_copies[k, h] = send(
            part.at[k, core_rows(1 - t % 2), halves[h]],
            from_core.at[k, :, halves[h]],
            one_send.at[i],
            one_recv.at[i],
            tp=core,
        )

    def add_core(k, h):
        one_copies[k, h].wait_recv()
        cols, i = halves[h], 2 * k + h
        for mine in (False, True):
            x = t // 2 if mine else 1 - t // 2
            base = pl.multiple_of((t % 2) * both + x * cap, cap)
            near = pl.multiple_of(x * cap, cap)
            total = part[k, pl.ds(base, cap), cols].astype(F32)
            total += from_core[k, pl.ds(near, cap), cols].astype(F32)
            if mine:
                kept[k, :, cols] = total
            else:
                to_chip[k, :, cols] = total.astype(BF16)
                two_copies[k, h] = send(
                    to_chip.at[k, :, cols],
                    from_chip.at[k, :, cols],
                    two_send.at[i],
                    two_recv.at[i],
                    tp=chip,
                )

    def add_chip(k, h):
        two_copies[k, h].wait_recv()
        cols, i = halves[h], 2 * k + h
        total = (kept[k, :, cols] + from_chip[k, :, cols].astype(F32)).astype(BF16)
        if k == 0:
            home[group_rows(s), cols] = total
        else:
            to_home[k, :, cols] = total
            home_copies[k, h] = send(
                to_home.at[k, :, cols],
                home.at[group_rows(s), cols],
                home_send.at[i],
                home_recv.at[i],
                sp=sp_of[k],
            )

    def halved(stage, k):
        stage(k, 0)
        stage(k, 1)

    def step(k):
        raise_units(k)
        halved(lower_units, k)

    for h in (0, 1):
        forward(1, h)
        pass_on(0, h)
    step(0)
    for h in (0, 1):
        forward(2, h)
        pass_on(1, h)
    step(1)
    for h in (0, 1):
        forward(3, h)
        pass_on(2, h)
    halved(add_core, 1)
    step(2)
    halved(pass_on, 3)
    halved(add_core, 2)
    halved(add_core, 0)
    halved(add_chip, 1)
    step(3)
    for h in (0, 1):
        add_core(3, h)
    halved(add_chip, 2)
    halved(add_chip, 0)
    halved(add_chip, 3)

    def finish(n, carry):
        cols = column(n)
        out[:, cols] = (stream[:, cols] + dot(back, home[:, cols])).astype(BF16)
        return carry

    for h in (0, 1):
        for k in (1, 2, 3):
            home_copies[k, h].wait_recv()
        lax.fori_loop(h * tiles // 2, (h + 1) * tiles // 2, finish, 0)
    for copy in pending:
        copy.wait_send()


def fused(*args):
    (conv_input, _, _, _, out_proj, residual, gain, _, _, w_gate, w_up, w_down) = args
    rows, width = residual.shape
    count, channels = conv_input.shape
    local, _, units = w_gate.shape
    cap = rows // GROUPS
    w_down = w_down.reshape(local * units, width)
    args = args[:6] + (gain.reshape(1, width), args[7].T, args[8].T) + args[9:11] + (w_down,)
    vmem = pl.BlockSpec(memory_space=pltpu.VMEM)
    far = pl.BlockSpec(memory_space=pl.ANY)
    sems = pltpu.SemaphoreType.DMA
    return pl.pallas_call(
        fused_kernel,
        out_shape=jax.ShapeDtypeStruct((rows, width), BF16),
        in_specs=[far] * 3 + [vmem] + [far] * 2 + [vmem] * 3 + [far] * 3,
        out_specs=vmem,
        scratch_shapes=[
            pltpu.VMEM((count, channels), BF16),
            pltpu.VMEM((count, channels), BF16),
            pltpu.VMEM((count, channels), BF16),
            pltpu.VMEM((rows, width), BF16),
            pltpu.VMEM(out_proj.shape, BF16),
            pltpu.VMEM(w_gate.shape, BF16),
            pltpu.VMEM(w_up.shape, BF16),
            pltpu.VMEM(w_down.shape, BF16),
            pltpu.VMEM((2, 16, channels), BF16),
            pltpu.VMEM((count + 8, channels), F32),
            pltpu.VMEM((3, rows, channels), BF16),
            pltpu.VMEM((4, rows, channels), BF16),
            pltpu.VMEM((rows, width), F32),
            pltpu.VMEM((rows, width + LANES), BF16),
            pltpu.VMEM((4, 4 * cap, width + LANES), BF16),
            pltpu.VMEM((4 * cap, local * units), BF16),
            pltpu.VMEM((4, 4 * cap, width), BF16),
            pltpu.VMEM((4, 2 * cap, width), BF16),
            pltpu.VMEM((4, cap, width), F32),
            pltpu.VMEM((4, cap, width), BF16),
            pltpu.VMEM((4, cap, width), BF16),
            pltpu.VMEM((4, cap, width), BF16),
            pltpu.VMEM((rows, width), BF16),
            sems((8,)),
            sems((2,)),
            sems((2,)),
            sems((3,)),
            sems((4,)),
        ]
        + [sems((8,))] * 14,
        compiler_params=pltpu.CompilerParams(
            collective_id=0, has_side_effects=True, vmem_limit_bytes=56 << 20
        ),
    )(*args)


def on_device(*args):
    residual, routes, w_gate = args[5], args[7], args[9]
    rows, local, seq_ranks = residual.shape[0], w_gate.shape[0], lax.axis_size("sp")
    dense = local == routes.shape[1] == 2 and local * seq_ranks == local * GROUPS
    if dense and lax.axis_size("tp") == 4 and rows % LANES == 0:
        return fused(*args)
    return generic(*args)


def solution(mesh):
    return jax.shard_map(
        on_device,
        mesh=mesh,
        in_specs=(
            P(("grp", "sp"), "tp"),
            P(("grp", "sp"), "tp"),
            P(("grp", "sp"), "tp"),
            P(),
            P(),
            P(("grp", "sp", "tp"), None),
            P(),
            P(("grp", "sp", "tp"), None),
            P(("grp", "sp", "tp"), None),
            P("sp", None, "tp"),
            P("sp", None, "tp"),
            P("sp", "tp", None),
        ),
        out_specs=P(("grp", "sp", "tp"), None),
        check_vma=False,
    )
```

```python
import functools

import jax
import jax.numpy as jnp
from jax import lax
from jax.experimental import pallas as pl
from jax.experimental.pallas import tpu as pltpu
from jax.sharding import PartitionSpec as P

GROUPS = 4
LANES = 128
F32, BF16 = jnp.float32, jnp.bfloat16


def shifted(block, axis, distance):
    devices = range(lax.axis_size(axis))
    route = [(i - distance, i) for i in devices if i - distance in devices]
    return lax.ppermute(block, axis, route)


def generic(
    conv_input,
    pre_gate,
    post_gate,
    conv_taps,
    out_proj,
    residual_in,
    norm_gain,
    routes,
    route_weight,
    w_gate,
    w_up,
    w_down,
):
    shards = lax.axis_size("tp")
    place = lax.axis_index("tp")
    seq_ranks = lax.axis_size("sp")
    channels = conv_input.shape[1]
    width = residual_in.shape[1]
    taps = lax.dynamic_slice_in_dim(conv_taps, place * channels, channels, 1)
    prior_input, prior_gate = shifted((conv_input[-2:], pre_gate[-2:]), "sp", 1)
    gated = jnp.concatenate(
        [
            prior_gate.astype(jnp.float32) * prior_input.astype(jnp.float32),
            pre_gate.astype(jnp.float32) * conv_input.astype(jnp.float32),
        ],
        axis=0,
    )
    conv = gated[2:] * taps[2] + gated[1:-1] * taps[1] + gated[:-2] * taps[0]
    mixed = (post_gate.astype(jnp.float32) * conv).astype(jnp.bfloat16)
    token_rows = lax.all_to_all(mixed, "tp", split_axis=0, concat_axis=1, tiled=True)
    projected = jnp.dot(token_rows, out_proj, preferred_element_type=jnp.float32)
    stream = residual_in.astype(jnp.float32) + projected
    scale = lax.rsqrt(jnp.mean(stream * stream, axis=-1, keepdims=True) + 1e-06)
    normed = (stream * scale * norm_gain).astype(jnp.bfloat16)
    block_rows = routes.shape[0]
    local_experts = w_gate.shape[0]
    experts = local_experts * seq_ranks
    capacity = 2 * block_rows // experts
    flat_routes = routes.reshape(-1)
    position = jnp.arange(flat_routes.shape[0], dtype=jnp.int32)
    earlier = (flat_routes[:, None] == flat_routes[None, :]) & (
        position[None, :] < position[:, None]
    )
    rank = jnp.sum(earlier.astype(jnp.int32), axis=1)
    slot = flat_routes * capacity + rank
    outgoing = (
        jnp.zeros((experts * capacity, width), jnp.bfloat16).at[slot].set(normed[position // 2])
    )
    outgoing = outgoing.reshape(seq_ranks, local_experts, capacity, width)
    spread = lax.all_gather(
        lax.all_to_all(outgoing, "sp", split_axis=0, concat_axis=0, tiled=True)[:, None],
        "tp",
        axis=1,
        tiled=True,
    )
    count = spread.shape[3]
    partials = []
    for expert in range(local_experts):
        rows = spread[:, :, expert].reshape(seq_ranks * shards * count, width)
        gate = jnp.dot(rows, w_gate[expert], preferred_element_type=jnp.float32)
        upper = jnp.dot(rows, w_up[expert], preferred_element_type=jnp.float32)
        hidden = (jax.nn.silu(gate) * upper).astype(jnp.bfloat16)
        part = jnp.dot(hidden, w_down[expert], preferred_element_type=jnp.float32).astype(
            jnp.bfloat16
        )
        partials.append(part.reshape(seq_ranks, shards, count, width))
    stacked = jnp.stack(partials, axis=2)
    summed = lax.psum_scatter(stacked, "tp", scatter_dimension=1, tiled=True).astype(jnp.float32)
    returned = lax.all_to_all(
        summed[:, 0].astype(jnp.bfloat16), "sp", split_axis=0, concat_axis=0, tiled=True
    )
    results = returned.reshape(experts * capacity, width)[slot]
    results = results.reshape(block_rows, 2, width).astype(jnp.float32)
    weighted = jnp.sum(route_weight[:, :, None] * results, axis=1)
    return (stream + weighted).astype(jnp.bfloat16)


def dot(a, b):
    return jnp.dot(a, b, preferred_element_type=F32)


def fused_kernel(
    input_hbm,
    pre_hbm,
    post_hbm,
    conv_taps,
    proj_hbm,
    residual_hbm,
    gain,
    routes,
    route_weight,
    gate_hbm,
    up_hbm,
    down_hbm,
    out,
    conv_input,
    pre_gate,
    post_gate,
    residual,
    proj,
    w_gate,
    w_up,
    w_down,
    halo,
    gated,
    mix_out,
    mix_in,
    stream,
    leaving,
    tok,
    hidden,
    part,
    from_core,
    kept,
    to_chip,
    from_chip,
    to_home,
    home,
    load_sem,
    halo_send,
    halo_recv,
    mix_send,
    mix_recv,
    z_send,
    z_recv,
    x_send,
    x_recv,
    c_send,
    c_recv,
    d_send,
    d_recv,
    one_send,
    one_recv,
    two_send,
    two_recv,
    home_send,
    home_recv,
):
    s, t = lax.axis_index("sp"), lax.axis_index("tp")
    rows, width = residual.shape
    channels = conv_input.shape[1]
    cap = rows // GROUPS
    units = w_gate.shape[2]
    core, chip, far = t + 1 - 2 * (t % 2), (t + 2) % 4, 3 - t
    sp_of = [s, s + 1 - 2 * (s % 2), (s + 2) % 4, 3 - s]
    pos = lambda place: (place % 2) * 2 + place // 2
    pending = []

    def send(src, dst, send_sem, recv_sem, **where):
        copy = pltpu.make_async_remote_copy(
            src_ref=src,
            dst_ref=dst,
            send_sem=send_sem,
            recv_sem=recv_sem,
            device_id=where,
            device_id_type=pl.DeviceIdType.MESH,
        )
        copy.start()
        pending.append(copy)
        return copy

    barrier = pltpu.get_barrier_semaphore()
    for other in (core, chip, far):
        pl.semaphore_signal(
            barrier, inc=1, device_id={"tp": other}, device_id_type=pl.DeviceIdType.MESH
        )
    for other in sp_of[1:]:
        pl.semaphore_signal(
            barrier, inc=1, device_id={"sp": other}, device_id_type=pl.DeviceIdType.MESH
        )
    loads = []
    for i, (a, b) in enumerate(
        (
            (input_hbm, conv_input),
            (pre_hbm, pre_gate),
            (post_hbm, post_gate),
            (residual_hbm, residual),
            (proj_hbm, proj),
            (gate_hbm, w_gate),
            (up_hbm, w_up),
            (down_hbm, w_down),
        )
    ):
        loads.append(pltpu.make_async_copy(a, b, load_sem.at[i]))
        loads[-1].start()

    first, second = routes[0:1, :], routes[1:2, :]
    epg = w_gate.shape[0]
    down = lax.broadcasted_iota(jnp.int32, (rows, rows), 0)
    across = lax.broadcasted_iota(jnp.int32, (rows, rows), 1)
    group = lax.broadcasted_iota(jnp.int32, (16, rows), 0)
    member = (first >= group * epg) & (first < group * epg + epg) & (group < GROUPS)
    member = jnp.where(member, 1.0, 0.0)
    earlier = jnp.where(down < across, 1.0, 0.0).astype(BF16)
    rank = dot(member.astype(BF16), earlier)
    slot = jnp.sum(member * (rank + (group * cap).astype(F32)), axis=0, keepdims=True)
    pick = jnp.where(slot == down.astype(F32), 1.0, 0.0)
    back = pick.T.astype(BF16)
    pick = pick.astype(BF16)
    low = jnp.where(first < second, route_weight[0:1, :], route_weight[1:2, :])
    high = jnp.where(first < second, route_weight[1:2, :], route_weight[0:1, :])
    low_top, high_top = low.astype(BF16).astype(F32), high.astype(BF16).astype(F32)
    line = lax.broadcasted_iota(jnp.int32, (LANES, rows), 0)
    scales = jnp.where(
        line == 0,
        low_top,
        jnp.where(
            line == 1,
            low - low_top,
            jnp.where(line == 2, high_top, jnp.where(line == 3, high - high_top, 0.0)),
        ),
    ).astype(BF16)
    scales = lax.dot_general(
        pick, scales, (((1,), (1,)), ((), ())), preferred_element_type=F32
    )
    leaving[:, pl.ds(width, LANES)] = scales.astype(BF16)

    loads[0].wait()
    loads[1].wait()
    pl.semaphore_wait(barrier, 6)

    count = conv_input.shape[0]
    halo_copies = [
        send(
            ref.at[pl.ds(count - 16, 16), :],
            halo.at[i],
            halo_send.at[i],
            halo_recv.at[i],
            sp=(s + 1) % 4,
        )
        for i, ref in enumerate((conv_input, pre_gate))
    ]
    gated[pl.ds(8, count), :] = pre_gate[...].astype(F32) * conv_input[...].astype(F32)
    taps = conv_taps[:, pl.ds(pl.multiple_of(t * channels, channels), channels)]
    loads[2].wait()

    def mix(place):
        start = pl.multiple_of(place * rows, rows)
        g = gated[pl.ds(start, rows + 8), :]
        conv = g[8:] * taps[2:3] + g[7:-1] * taps[1:2] + g[6:-2] * taps[0:1]
        return (post_gate[pl.ds(start, rows), :].astype(F32) * conv).astype(BF16)

    def send_mixed(i, place):
        mix_out[i] = mix(place)
        send(mix_out.at[i], mix_in.at[t], mix_send.at[i], mix_recv.at[t], tp=place)

    def wait_mixed(place):
        pltpu.make_async_remote_copy(
            src_ref=mix_in.at[place],
            dst_ref=mix_in.at[place],
            send_sem=mix_send.at[0],
            recv_sem=mix_recv.at[place],
            device_id={"tp": place},
            device_id_type=pl.DeviceIdType.MESH,
        ).wait_recv()

    across_chip = 2 * (1 - t // 2)
    send_mixed(0, across_chip + 1)
    for copy in halo_copies:
        copy.wait_recv()
    before = halo[0, 8:16, :].astype(F32) * halo[1, 8:16, :].astype(F32)
    gated[0:8, :] = jnp.where(s > 0, before, 0.0)
    send_mixed(1, across_chip)
    send_mixed(2, core)
    mix_in[t] = mix(t)

    tile = 512
    tiles = width // tile
    column = lambda n: pl.ds(pl.multiple_of(n * tile, tile), tile)
    weights_of = lambda place: pl.ds(pl.multiple_of(place * channels, channels), channels)
    loads[3].wait()
    loads[4].wait()
    wait_mixed(core)

    def project_near(n, carry):
        cols = column(n)
        total = residual[:, cols].astype(F32)
        for place in (t, core):
            total += dot(mix_in[place], proj[weights_of(place), cols])
        stream[:, cols] = total
        return carry

    lax.fori_loop(0, tiles, project_near, 0)
    wait_mixed(chip)
    wait_mixed(far)

    def project_far(n, squares):
        cols = column(n)
        total = stream[:, cols]
        for place in (chip, far):
            total += dot(mix_in[place], proj[weights_of(place), cols])
        stream[:, cols] = total
        return squares + jnp.sum(total * total, axis=1, keepdims=True)

    squares = lax.fori_loop(0, tiles, project_far, jnp.zeros((rows, 1), F32))
    scale = lax.rsqrt(squares / width + 1e-06)

    def norm(n, carry):
        cols = column(n)
        row = (stream[:, cols] * scale * gain[:, cols]).astype(BF16)
        leaving[:, cols] = dot(pick, row).astype(BF16)
        return carry

    lax.fori_loop(0, tiles, norm, 0)

    some = cap // 2
    group_rows = lambda g: pl.ds(pl.multiple_of(g * cap, cap), cap)
    part_rows = lambda g, h: pl.ds(pl.multiple_of(g * cap + h * some, some), some)
    block = lambda place: pl.ds(pl.multiple_of(pos(place) * some, some), some)
    z_copies, x_copies, c_copies, d_copies = {}, {}, {}, {}
    one_copies, two_copies, home_copies = {}, {}, {}

    def forward(k, h):
        src = leaving.at[part_rows(s, h), :]
        if k:
            z_copies[k, h].wait_recv()
            src = tok.at[sp_of[k], h, block(t), :]
        dst = tok.at[sp_of[k], h, block(t), :]
        i = 2 * k + h
        x_copies[k, h] = send(src, dst, x_send.at[i], x_recv.at[i], tp=chip)
        c_copies[k, h] = send(src, dst, c_send.at[i], c_recv.at[i], tp=core)

    def pass_on(k, h):
        x_copies[k, h].wait_recv()
        i = 2 * k + h
        arrived = tok.at[sp_of[k], h, block(chip), :]
        d_copies[k, h] = send(arrived, arrived, d_send.at[i], d_recv.at[i], tp=core)

    for k, h in ((1, 0), (1, 1), (2, 0), (2, 1), (3, 0), (3, 1)):
        i = 2 * k + h
        z_copies[k, h] = send(
            leaving.at[part_rows(sp_of[k], h), :],
            tok.at[s, h, block(t), :],
            z_send.at[i],
            z_recv.at[i],
            sp=sp_of[k],
        )
    for h in (0, 1):
        forward(0, h)
        tok[s, h, block(t), :] = leaving[part_rows(s, h), :]
    for load in loads[5:]:
        load.wait()

    def experts(k, *one):
        own = one or (0, 1)
        for h in own:
            c_copies[k, h].wait_recv()
            d_copies[k, h].wait_recv()
        g, low_half, m = sp_of[k], own[0], len(own)
        where, length = pl.ds(low_half, m), m * 2 * cap
        x = tok[g, where, :, 0:width].reshape(length, width)
        top = tok[g, where, :, pl.ds(width, LANES)].reshape(length, LANES).astype(F32)
        for e in range(epg):
            w = top[:, 2 * e : 2 * e + 1] + top[:, 2 * e + 1 : 2 * e + 2]
            gate = dot(x, w_gate[e])
            upper = dot(x, w_up[e])
            act = gate / (1.0 + jnp.exp(-gate)) * upper * w
            hidden[0:length, pl.ds(e * units, units)] = act.astype(BF16)

        def lower(n, carry):
            cols = column(n)
            rows_out = dot(hidden[0:length, :], w_down[:, cols]).astype(BF16)
            part[k, where, :, cols] = rows_out.reshape(m, 2 * cap, tile)
            return carry

        lax.fori_loop(0, tiles, lower, 0)
        for h in own:
            i = 2 * k + h
            one_copies[k, h] = send(
                part.at[k, h, core_rows(1 - t % 2), :],
                from_core.at[k, h],
                one_send.at[i],
                one_recv.at[i],
                tp=core,
            )

    core_rows = lambda c: pl.ds(pl.multiple_of(c * cap, cap), cap)

    def add_core(k, h):
        one_copies[k, h].wait_recv()
        i = 2 * k + h
        for mine in (False, True):
            x = t // 2 if mine else 1 - t // 2
            base = pl.multiple_of((t % 2) * cap + x * some, some)
            near = pl.multiple_of(x * some, some)
            total = part[k, h, pl.ds(base, some), :].astype(F32)
            total += from_core[k, h, pl.ds(near, some), :].astype(F32)
            if mine:
                kept[k, h] = total
            else:
                to_chip[k, h] = total.astype(BF16)
                two_copies[k, h] = send(
                    to_chip.at[k, h],
                    from_chip.at[k, h],
                    two_send.at[i],
                    two_recv.at[i],
                    tp=chip,
                )

    def add_chip(k, h):
        two_copies[k, h].wait_recv()
        i = 2 * k + h
        total = (kept[k, h] + from_chip[k, h].astype(F32)).astype(BF16)
        if k == 0:
            home[part_rows(s, h), :] = total
        else:
            to_home[k, h] = total
            home_copies[k, h] = send(
                to_home.at[k, h],
                home.at[part_rows(s, h), :],
                home_send.at[i],
                home_recv.at[i],
                sp=sp_of[k],
            )

    stages = dict(F=forward, P=pass_on, C=experts, A=add_core, B=add_chip)
    order = (
        "F10 P00 F11 P01",
        "C0 F20 P10 F21",
        "P11 C1 F30 P20",
        "F31 P21 A10 A11",
        "C2 P30 P31 A20",
        "A21 B10 B11 C3",
        "A30 A31 B20 B21",
        "A00 A01 B30 B31",
        "B00 B01",
    )
    for line_of in order:
        for stage in line_of.split():
            stages[stage[0]](*map(int, stage[1:]))

    def finish(n, carry):
        cols = column(n)
        out[:, cols] = (stream[:, cols] + dot(back, home[:, cols])).astype(BF16)
        return carry

    for copy in home_copies.values():
        copy.wait_recv()
    lax.fori_loop(0, tiles, finish, 0)
    for copy in pending:
        copy.wait_send()


def fused(*args):
    (conv_input, _, _, _, out_proj, residual, gain, _, _, w_gate, w_up, w_down) = args
    rows, width = residual.shape
    count, channels = conv_input.shape
    local, _, units = w_gate.shape
    cap = rows // GROUPS
    w_down = w_down.reshape(local * units, width)
    args = args[:6] + (gain.reshape(1, width), args[7].T, args[8].T) + args[9:11] + (w_down,)
    vmem = pl.BlockSpec(memory_space=pltpu.VMEM)
    far = pl.BlockSpec(memory_space=pl.ANY)
    sems = pltpu.SemaphoreType.DMA
    return pl.pallas_call(
        fused_kernel,
        out_shape=jax.ShapeDtypeStruct((rows, width), BF16),
        in_specs=[far] * 3 + [vmem] + [far] * 2 + [vmem] * 3 + [far] * 3,
        out_specs=vmem,
        scratch_shapes=[
            pltpu.VMEM((count, channels), BF16),
            pltpu.VMEM((count, channels), BF16),
            pltpu.VMEM((count, channels), BF16),
            pltpu.VMEM((rows, width), BF16),
            pltpu.VMEM(out_proj.shape, BF16),
            pltpu.VMEM(w_gate.shape, BF16),
            pltpu.VMEM(w_up.shape, BF16),
            pltpu.VMEM(w_down.shape, BF16),
            pltpu.VMEM((2, 16, channels), BF16),
            pltpu.VMEM((count + 8, channels), F32),
            pltpu.VMEM((3, rows, channels), BF16),
            pltpu.VMEM((4, rows, channels), BF16),
            pltpu.VMEM((rows, width), F32),
            pltpu.VMEM((rows, width + LANES), BF16),
            pltpu.VMEM((4, 2, 2 * cap, width + LANES), BF16),
            pltpu.VMEM((4 * cap, local * units), BF16),
            pltpu.VMEM((4, 2, 2 * cap, width), BF16),
            pltpu.VMEM((4, 2, cap, width), BF16),
            pltpu.VMEM((4, 2, cap // 2, width), F32),
            pltpu.VMEM((4, 2, cap // 2, width), BF16),
            pltpu.VMEM((4, 2, cap // 2, width), BF16),
            pltpu.VMEM((4, 2, cap // 2, width), BF16),
            pltpu.VMEM((rows, width), BF16),
            sems((8,)),
            sems((2,)),
            sems((2,)),
            sems((3,)),
            sems((4,)),
        ]
        + [sems((8,))] * 14,
        compiler_params=pltpu.CompilerParams(
            collective_id=0, has_side_effects=True, vmem_limit_bytes=56 << 20
        ),
    )(*args)


def on_device(*args):
    residual, routes, w_gate = args[5], args[7], args[9]
    rows, local, seq_ranks = residual.shape[0], w_gate.shape[0], lax.axis_size("sp")
    dense = local == routes.shape[1] == 2 and local * seq_ranks == local * GROUPS
    if dense and lax.axis_size("tp") == 4 and rows % LANES == 0:
        return fused(*args)
    return generic(*args)


def solution(mesh):
    return jax.shard_map(
        on_device,
        mesh=mesh,
        in_specs=(
            P(("grp", "sp"), "tp"),
            P(("grp", "sp"), "tp"),
            P(("grp", "sp"), "tp"),
            P(),
            P(),
            P(("grp", "sp", "tp"), None),
            P(),
            P(("grp", "sp", "tp"), None),
            P(("grp", "sp", "tp"), None),
            P("sp", None, "tp"),
            P("sp", None, "tp"),
            P("sp", "tp", None),
        ),
        out_specs=P(("grp", "sp", "tp"), None),
        check_vma=False,
    )
```
